32 devices in a mesh: kv: 8 (over z, x), tp: 4 (over y, core).
Axes of the slice: x: 2, y: 2, z: 4, core: 2. Of those that a mesh axis runs over, the one named last changes fastest.
Arguments:
- tokens: bfloat16 [16384, 2048], P('kv'), may hold values from -6 to 6
- norm_gain: bfloat16 [2048], replicated, may hold values from 0.099609375 to 1.8984375
- query_weight: bfloat16 [2048, 1024], P(None, 'tp'), may hold values from -0.125 to 0.125
- cmp_key_weight: bfloat16 [2048, 512], P(None, 'tp'), may hold values from -0.125 to 0.125
- cmp_value_weight: bfloat16 [2048, 512], P(None, 'tp'), may hold values from -0.125 to 0.125
- sel_key_weight: bfloat16 [2048, 512], P(None, 'tp'), may hold values from -0.125 to 0.125
- sel_value_weight: bfloat16 [2048, 512], P(None, 'tp'), may hold values from -0.125 to 0.125
- branch_weight: bfloat16 [2, 2048, 16], replicated, may hold values from -0.125 to 0.125
- key_embed: bfloat16 [8, 32, 64], P('tp'), may hold values from -3 to 3
- key_inner: bfloat16 [8, 2048, 64], P('tp'), may hold values from -0.125 to 0.125
- key_outer: bfloat16 [8, 64, 64], P('tp'), may hold values from -0.75 to 0.75
- value_embed: bfloat16 [8, 32, 64], P('tp'), may hold values from -3 to 3
- value_inner: bfloat16 [8, 2048, 64], P('tp'), may hold values from -0.125 to 0.125
- value_outer: bfloat16 [8, 64, 64], P('tp'), may hold values from -0.75 to 0.75
- out_weight: bfloat16 [1024, 2048], replicated, may hold values from -0.1875 to 0.1875
- chosen: int32 [8, 128, 8], P('tp'), may hold values from 0 to 255, as said below
Outputs:
- attended: bfloat16 [16384, 2048], P(('kv', 'tp'))
The draws below stay inside these ranges and needn't reach their ends.
Inputs may be any that keep to these rules, and one draw needn't show every extreme that they name: `chosen`: each entry is the index of a block of 64 positions in the whole sequence. For every key head and query block, its 8 entries lie in 8 different aligned spans of 2048 positions (at most one from any span), and none lies inside the query block's own positions.
All inputs are finite; a program needn't handle non-finite values.
Results may differ from the reference program's by a relative error of at most 0.0075.
Values may be sent and summed in bfloat16 or wider, within the bound.
A program may use at most 128 MiB of HBM per device.

```python
import jax
import jax.numpy as jnp
from jax import lax

D = 2048
HEADS = 16
KV_HEADS = 8
HEAD_DIM = 64
CMP_BLOCK = 32
SEL_BLOCK = 64
Q_BLOCK = 128
FAR_PICKS = 8
TOK_DEV = 2048
SEQ = 16384


def draw_chosen(key, part):
    interval_limits = SEQ // TOK_DEV
    per_span = TOK_DEV // Q_BLOCK
    span_blocks = TOK_DEV // SEL_BLOCK
    own_blocks = Q_BLOCK // SEL_BLOCK
    query_blocks = SEQ // Q_BLOCK
    key_noise, key_inner, key_shift = jax.random.split(key, 3)
    diagonal_group = jnp.arange(query_blocks, dtype=jnp.int32) // per_span
    local_index = jnp.arange(query_blocks, dtype=jnp.int32) % per_span
    eligible_group = jnp.arange(interval_limits, dtype=jnp.int32)
    jitter_perturbation = jax.random.randint(key_noise, (KV_HEADS, query_blocks, interval_limits), 0, 2 ** 16)
    preference_increment = jnp.where(eligible_group[None, :] <= diagonal_group[:, None], 2 ** 24, 0)
    preference_increment = preference_increment + jnp.where(eligible_group[None, :] == diagonal_group[:, None] - 1, 2 ** 26, 0)
    preference_increment = preference_increment + jnp.where(eligible_group[None, :] == diagonal_group[:, None] - interval_limits // 2, 2 ** 26, 0)
    preference_increment = preference_increment + jnp.where(eligible_group[None, :] == 0, 2 ** 25, 0)
    group_relevance = jitter_perturbation * interval_limits + eligible_group[None, None, :] + preference_increment[None]
    _, picked = lax.top_k(group_relevance, FAR_PICKS)
    inside = jax.random.randint(key_inner, (KV_HEADS, query_blocks, FAR_PICKS), 0, span_blocks)
    offset = jax.random.randint(key_shift, (KV_HEADS, query_blocks, FAR_PICKS), 0, span_blocks - own_blocks)
    shifted = (local_index[None, :, None] * own_blocks + own_blocks + offset) % span_blocks
    within = jnp.where(picked == diagonal_group[None, :, None], shifted, inside)
    return (picked * span_blocks + within).astype(jnp.int32)


def block_scale(rng, dims, pieces, smallest, top_value):
    def one(axis_at, blocks):
        draws = jax.random.uniform(jax.random.fold_in(jax.random.fold_in(rng, 6), axis_at), (blocks,), jnp.float32, smallest / len(pieces), top_value / len(pieces))
        return jnp.repeat(jnp.exp(draws), dims[axis_at] // blocks).reshape((-1,) + (1,) * (len(dims) - axis_at - 1))

    factor_of = one(*pieces[0])
    for cut in pieces[1:]:
        factor_of = factor_of * one(*cut)
    return factor_of


def bell_draw(own_key, shape, scale, bound, cuts=(), kind=jnp.bfloat16):
    level = block_scale(own_key, shape, cuts, -0.22, 0.18) if cuts else 1.0
    result = jax.random.normal(own_key, shape, jnp.float32) * scale * level
    return jnp.minimum(jnp.maximum(result, -bound), bound).astype(kind)


def setup_inputs(seed: int = 0) -> dict:
    splits = jax.random.split(jax.random.key(seed), 17)
    return {
        "tokens": bell_draw(splits[0], (SEQ, D), 1.0, 6.0, ((0, 8),)),
        "norm_gain": jnp.clip(1.0 + 0.18 * jax.random.normal(splits[1], (D,), jnp.float32), 0.099609375, 1.8984375).astype(jnp.bfloat16),
        "query_weight": bell_draw(splits[2], (D, HEADS * HEAD_DIM), D ** -0.5, 0.125, ((1, 4),)),
        "cmp_key_weight": bell_draw(splits[3], (D, KV_HEADS * HEAD_DIM), D ** -0.5, 0.125, ((1, 4),)),
        "cmp_value_weight": bell_draw(splits[4], (D, KV_HEADS * HEAD_DIM), D ** -0.5, 0.125, ((1, 4),)),
        "sel_key_weight": bell_draw(splits[5], (D, KV_HEADS * HEAD_DIM), D ** -0.5, 0.125, ((1, 4),)),
        "sel_value_weight": bell_draw(splits[6], (D, KV_HEADS * HEAD_DIM), D ** -0.5, 0.125, ((1, 4),)),
        "branch_weight": bell_draw(splits[7], (2, D, HEADS), D ** -0.5, 0.125),
        "key_embed": bell_draw(splits[8], (KV_HEADS, CMP_BLOCK, HEAD_DIM), 0.5, 3.0, ((0, 4),)),
        "key_inner": bell_draw(splits[9], (KV_HEADS, CMP_BLOCK * HEAD_DIM, HEAD_DIM), (CMP_BLOCK * HEAD_DIM) ** -0.5, 0.125, ((0, 4),)),
        "key_outer": bell_draw(splits[10], (KV_HEADS, HEAD_DIM, HEAD_DIM), HEAD_DIM ** -0.5, 0.75, ((0, 4),)),
        "value_embed": bell_draw(splits[11], (KV_HEADS, CMP_BLOCK, HEAD_DIM), 0.5, 3.0, ((0, 4),)),
        "value_inner": bell_draw(splits[12], (KV_HEADS, CMP_BLOCK * HEAD_DIM, HEAD_DIM), (CMP_BLOCK * HEAD_DIM) ** -0.5, 0.125, ((0, 4),)),
        "value_outer": bell_draw(splits[13], (KV_HEADS, HEAD_DIM, HEAD_DIM), HEAD_DIM ** -0.5, 0.75, ((0, 4),)),
        "out_weight": bell_draw(splits[14], (HEADS * HEAD_DIM, D), (HEADS * HEAD_DIM) ** -0.5, 0.1875),
        "chosen": draw_chosen(jax.random.fold_in(splits[16], 71), 0),
    }


ROPE_BASE = 10000.0
norm_eps = 1e-06
masked_score = -1000000000.0

def rotate(values_in, positions):
    half_dim = values_in.shape[-1] // 2
    inverse = ROPE_BASE ** (-jnp.arange(half_dim, dtype=jnp.float32) / half_dim)
    rotary_phases = positions.astype(jnp.float32)[:, None] * inverse[None, :]
    cosine = jnp.cos(rotary_phases)[:, None, :]
    sine = jnp.sin(rotary_phases)[:, None, :]
    first_half = values_in[..., :half_dim]
    second_half = values_in[..., half_dim:]
    return jnp.concatenate([first_half * cosine - second_half * sine, second_half * cosine + first_half * sine], axis=-1)

def summarize(raw_rows, embed, inner, outer):
    block_count = raw_rows.shape[0] // CMP_BLOCK
    blocked = raw_rows.reshape(block_count, CMP_BLOCK, KV_HEADS, HEAD_DIM).transpose(2, 0, 1, 3).astype(jnp.float32)
    blocked = (blocked + embed.astype(jnp.float32)[:, None]).astype(jnp.bfloat16)
    blocked = blocked.reshape(KV_HEADS, block_count, CMP_BLOCK * HEAD_DIM)
    hidden = jax.nn.gelu(jnp.einsum('knc,kce->kne', blocked.astype(jnp.float32), inner.astype(jnp.float32))).astype(jnp.bfloat16)
    return jnp.einsum('kne,kef->knf', hidden.astype(jnp.float32), outer.astype(jnp.float32)).astype(jnp.bfloat16)

def reference(tokens, norm_gain, query_weight, cmp_key_weight, cmp_value_weight, sel_key_weight, sel_value_weight, branch_weight, key_embed, key_inner, key_outer, value_embed, value_inner, value_outer, out_weight, chosen):
    length = tokens.shape[0]
    group_size = HEADS // KV_HEADS
    positions = jnp.arange(length, dtype=jnp.int32)
    scale = HEAD_DIM ** (-0.5)
    expanded_mask = tokens.astype(jnp.float32)
    normed = (expanded_mask * lax.rsqrt(lax.optimization_barrier(jnp.mean(expanded_mask * expanded_mask, axis=-1, keepdims=True)) + norm_eps) * norm_gain.astype(jnp.float32)).astype(jnp.bfloat16)

    def project(weight_in):
        return jnp.dot(normed, weight_in, preferred_element_type=jnp.float32)
    query = project(query_weight).reshape(length, HEADS, HEAD_DIM)
    q_plain = query.astype(jnp.bfloat16)
    q_turn = rotate(query, positions).astype(jnp.bfloat16)
    cmp_key = project(cmp_key_weight).astype(jnp.bfloat16).reshape(length, KV_HEADS, HEAD_DIM)
    cmp_value = project(cmp_value_weight).astype(jnp.bfloat16).reshape(length, KV_HEADS, HEAD_DIM)
    sel_key = rotate(project(sel_key_weight).reshape(length, KV_HEADS, HEAD_DIM), positions).astype(jnp.bfloat16)
    selected_value = project(sel_value_weight).astype(jnp.bfloat16).reshape(length, KV_HEADS, HEAD_DIM)
    gate_cmp = jax.nn.sigmoid(project(branch_weight[0]))
    gate_sel = jax.nn.sigmoid(project(branch_weight[1]))
    summary_key = summarize(cmp_key, key_embed, key_inner, key_outer)
    summary_value = summarize(cmp_value, value_embed, value_inner, value_outer)
    summary_count = summary_key.shape[1]
    block_end = (jnp.arange(summary_count, dtype=jnp.int32) + 1) * CMP_BLOCK - 1

    def compress_head(packed_rows):
        head_query, head_keys, head_values = packed_rows
        scores = jnp.einsum('tgd,cd->tgc', head_query.astype(jnp.float32), head_keys.astype(jnp.float32)) * scale
        allowed_keys = (block_end[None, :] <= positions[:, None])[:, None, :]
        probs = jax.nn.softmax(jnp.where(allowed_keys, scores, masked_score), axis=-1) * allowed_keys.astype(jnp.float32)
        return jnp.einsum('tgc,cd->tgd', probs.astype(jnp.bfloat16).astype(jnp.float32), head_values.astype(jnp.float32))
    q_group = q_plain.reshape(length, KV_HEADS, group_size, HEAD_DIM).transpose(1, 0, 2, 3)
    out_cmp = lax.map(compress_head, (q_group, summary_key, summary_value))
    out_cmp = out_cmp.transpose(1, 0, 2, 3).reshape(length, HEADS, HEAD_DIM)
    query_blocks = length // Q_BLOCK
    block_pos = jnp.arange(query_blocks, dtype=jnp.int32)[:, None] * Q_BLOCK + jnp.arange(Q_BLOCK, dtype=jnp.int32)[None, :]

    def select_head(packed_rows):
        head_query, head_keys, head_values, head_picks = packed_rows
        far_keys = head_keys.reshape(-1, SEL_BLOCK, HEAD_DIM)[head_picks].reshape(query_blocks, FAR_PICKS * SEL_BLOCK, HEAD_DIM)
        far_values = head_values.reshape(-1, SEL_BLOCK, HEAD_DIM)[head_picks].reshape(query_blocks, FAR_PICKS * SEL_BLOCK, HEAD_DIM)
        all_keys = jnp.concatenate([head_keys.reshape(query_blocks, Q_BLOCK, HEAD_DIM), far_keys], axis=1)
        all_values = jnp.concatenate([head_values.reshape(query_blocks, Q_BLOCK, HEAD_DIM), far_values], axis=1)
        far_pos = (head_picks[:, :, None] * SEL_BLOCK + jnp.arange(SEL_BLOCK, dtype=jnp.int32)[None, None, :]).reshape(query_blocks, -1)
        key_pos = jnp.concatenate([block_pos, far_pos], axis=1)
        allowed_keys = key_pos[:, None, None, :] <= block_pos[:, :, None, None]
        scores = jnp.einsum('nqgd,nmd->nqgm', head_query.astype(jnp.float32), all_keys.astype(jnp.float32)) * scale
        probs = jax.nn.softmax(jnp.where(allowed_keys, scores, masked_score), axis=-1)
        return jnp.einsum('nqgm,nmd->nqgd', probs.astype(jnp.bfloat16).astype(jnp.float32), all_values.astype(jnp.float32))
    q_sel = q_turn.reshape(query_blocks, Q_BLOCK, KV_HEADS, group_size, HEAD_DIM).transpose(2, 0, 1, 3, 4)
    out_sel = lax.map(select_head, (q_sel, sel_key.transpose(1, 0, 2), selected_value.transpose(1, 0, 2), chosen.astype(jnp.int32)))
    out_sel = out_sel.transpose(1, 2, 0, 3, 4).reshape(length, HEADS, HEAD_DIM)
    mixed = (gate_cmp[..., None] * out_cmp + gate_sel[..., None] * out_sel).reshape(length, HEADS * HEAD_DIM).astype(jnp.bfloat16)
    return jnp.dot(mixed, out_weight, preferred_element_type=jnp.float32).astype(jnp.bfloat16)
```

```python
import functools

import jax
import jax.numpy as jnp
from jax import lax
from jax.experimental import pallas as pl
from jax.experimental.pallas import tpu as pltpu
from jax.sharding import PartitionSpec as P

HEAD_DIM = 64
CMP_BLOCK = 32
SEL_BLOCK = 64
Q_BLOCK = 128
FAR_PICKS = 8
LANES = 2 * HEAD_DIM
PLANES = 4

ROPE_BASE = 10000.0
norm_eps = 1e-06
MASKED = -1e30


def params(n_axes, limit=48):
    return pltpu.CompilerParams(
        dimension_semantics=("arbitrary",) * n_axes, vmem_limit_bytes=limit * 1024 * 1024
    )


def norm_rows(tok_ref, gain_ref):
    x = tok_ref[...].astype(jnp.float32)
    inv = lax.rsqrt(jnp.mean(x * x, axis=-1, keepdims=True) + norm_eps)
    return (x * inv * gain_ref[...].astype(jnp.float32)).astype(jnp.bfloat16)


def turn(x, cosine, sine_up, sine_down):
    quarter = HEAD_DIM // 2
    return (
        x * cosine
        + pltpu.roll(x, LANES - quarter, 1) * sine_up
        + pltpu.roll(x, quarter, 1) * sine_down
    )


def low_lanes(shape):
    return lax.broadcasted_iota(jnp.int32, shape, 1) < HEAD_DIM


def sel_kernel(tok_ref, gain_ref, w_ref, cos_ref, up_ref, down_ref, *outs):
    normed = norm_rows(tok_ref, gain_ref)
    y = jnp.dot(normed, w_ref[...], preferred_element_type=jnp.float32)
    for k, out in enumerate(outs):
        x = y[:, k * LANES : (k + 1) * LANES]
        low = low_lanes(x.shape)
        turned = turn(x, cos_ref[...], up_ref[...], down_ref[...])
        out[...] = jnp.where(low, turned, x).astype(jnp.bfloat16)


def mid_kernel(
    tok_ref,
    gain_ref,
    w_ref,
    cos_ref,
    up_ref,
    down_ref,
    qp_ref,
    qt_ref,
    ck_ref,
    cv_ref,
    gate_ref,
):
    scale = HEAD_DIM ** (-0.5)
    normed = norm_rows(tok_ref, gain_ref)
    y = jnp.dot(normed, w_ref[...], preferred_element_type=jnp.float32)
    kv_local = qp_ref.shape[0]
    for k in range(kv_local):
        x = y[:, k * LANES : (k + 1) * LANES]
        low = low_lanes(x.shape)
        turned = turn(x, cos_ref[...], up_ref[...], down_ref[...]) * scale
        plain = x * scale
        for ref, v in ((qp_ref, plain), (qt_ref, turned)):
            ref[k, 0] = jnp.where(low, v, 0.0).astype(jnp.bfloat16)
            ref[k, 1] = jnp.where(low, pltpu.roll(v, HEAD_DIM, 1), 0.0).astype(jnp.bfloat16)
    base = kv_local * LANES
    width = kv_local * HEAD_DIM
    ck_ref[...] = y[:, base : base + width].astype(jnp.bfloat16).astype(jnp.float32)
    cv_ref[...] = y[:, base + width : base + 2 * width].astype(jnp.bfloat16).astype(jnp.float32)
    gate_ref[...] = jax.nn.sigmoid(y[:, base + 2 * width :])


def summary_kernel(ck_ref, cv_ref, ke_ref, ki_ref, ko_ref, ve_ref, vi_ref, vo_ref, out_ref):
    blocks = ck_ref.shape[0] // CMP_BLOCK

    def one(x_ref, e_ref, i_ref, o_ref):
        rows = []
        for c in range(CMP_BLOCK):
            part = x_ref[pl.ds(c, blocks, stride=CMP_BLOCK), :] + e_ref[c : c + 1, :]
            rows.append(part.astype(jnp.bfloat16))
        flat = jnp.concatenate(rows, axis=1)
        hidden = jnp.dot(flat, i_ref[...], preferred_element_type=jnp.float32)
        hidden = jax.nn.gelu(hidden).astype(jnp.bfloat16)
        return jnp.dot(hidden, o_ref[...], preferred_element_type=jnp.float32)

    sk = one(ck_ref, ke_ref, ki_ref, ko_ref)
    sv = one(cv_ref, ve_ref, vi_ref, vo_ref)
    for k in range(out_ref.shape[0]):
        at = slice(k * HEAD_DIM, (k + 1) * HEAD_DIM)
        out_ref[k] = jnp.concatenate([sk[:, at], sv[:, at]], axis=1).astype(jnp.bfloat16)


def nt_dot(a, b):
    return lax.dot_general(a, b, (((1,), (1,)), ((), ())), preferred_element_type=jnp.float32)


def gate_lanes(gate, first, shape):
    return jnp.where(low_lanes(shape), gate[:, first : first + 1], gate[:, first + 1 : first + 2])


def merge(out, rows):
    low = low_lanes((rows, LANES))
    return jnp.where(low, pltpu.roll(out[:rows], HEAD_DIM, 1), out[rows:])


def cmp_kernel(start_ref, q_ref, gate_ref, *rest):
    sums, out_ref = rest[:-1], rest[-1]
    rows = q_ref.shape[2]
    per = sums[0].shape[1]
    start = start_ref[0]
    tile_at = pl.program_id(0) * rows
    kv_local = q_ref.shape[0]
    lane = lax.broadcasted_iota(jnp.int32, (1, per * len(sums)), 1)
    ends = jnp.zeros_like(lane)
    for a in range(len(sums)):
        first = start_ref[a + 1]
        local = (lane - a * per + 1) * CMP_BLOCK - 1 + first
        local = jnp.where(first < 0, jnp.int32(2**30), local)
        ends = jnp.where((lane >= a * per) & (lane < (a + 1) * per), local, ends)
    row = lax.broadcasted_iota(jnp.int32, (2 * rows, 1), 0)
    pos = start + tile_at + jnp.where(row >= rows, row - rows, row)
    allowed = ends <= pos
    for k in range(kv_local):
        keys = jnp.concatenate([s[k] for s in sums], axis=0)
        q = jnp.concatenate([q_ref[k, 0], q_ref[k, 1]], axis=0)
        s = jnp.where(allowed, nt_dot(q, keys), MASKED)
        top = jnp.max(s, axis=-1, keepdims=True)
        e = jnp.where(allowed, jnp.exp(s - top), 0.0)
        total = jnp.sum(e, axis=-1, keepdims=True)
        o = jnp.dot(e.astype(jnp.bfloat16), keys, preferred_element_type=jnp.float32)
        o = o * jnp.where(total > 0.0, 1.0 / jnp.where(total > 0.0, total, 1.0), 0.0)
        o = merge(o, rows)
        g = gate_lanes(gate_ref[...], 2 * k, o.shape)
        out_ref[k] = o * g


def chosen_kernel(head, idx_ref, bias_ref, q_ref, gate_ref, oc_ref, *rest):
    stores, out_ref = rest[:-1], rest[-1]
    j = pl.program_id(0)
    own = stores[0][pl.ds(pl.multiple_of(j * Q_BLOCK, Q_BLOCK), Q_BLOCK), :]
    parts = [own]
    for a, store in enumerate(stores):
        at = pl.multiple_of(idx_ref[j * len(stores) + a] * SEL_BLOCK, SEL_BLOCK)
        parts.append(store[pl.ds(at, SEL_BLOCK), :])
    keys = jnp.concatenate(parts, axis=0)
    q = jnp.concatenate([q_ref[0, 0], q_ref[0, 1]], axis=0)
    s = nt_dot(q, keys) + bias_ref[0]
    row = lax.broadcasted_iota(jnp.int32, s.shape, 0)
    row = jnp.where(row >= Q_BLOCK, row - Q_BLOCK, row)
    lane = lax.broadcasted_iota(jnp.int32, s.shape, 1)
    s = jnp.where((lane < Q_BLOCK) & (lane > row), MASKED, s)
    top = jnp.max(s, axis=-1, keepdims=True)
    e = jnp.exp(s - top)
    total = jnp.sum(e, axis=-1, keepdims=True)
    o = jnp.dot(e.astype(jnp.bfloat16), keys, preferred_element_type=jnp.float32) / total
    o = merge(o, Q_BLOCK)
    g = gate_lanes(gate_ref[...], gate_ref.shape[1] // 2 + 2 * head, o.shape)
    out_ref[...] = (oc_ref[0] + o * g).astype(jnp.bfloat16)


def cost(flops, moved):
    return pl.CostEstimate(flops=int(flops), bytes_accessed=int(moved), transcendentals=0)


def block_diagonal(w):
    n, a, b = w.shape
    zero = jnp.zeros((a, b), w.dtype)
    return jnp.concatenate(
        [jnp.concatenate([w[i] if i == j else zero for j in range(n)], axis=1) for i in range(n)],
        axis=0,
    )


def inner_diagonal(w):
    n, rows, e = w.shape
    w = w.reshape(n, CMP_BLOCK, HEAD_DIM, e)
    zero = jnp.zeros_like(w[0])
    full = jnp.stack(
        [jnp.concatenate([w[i] if i == j else zero for j in range(n)], axis=-1) for i in range(n)],
        axis=1,
    )
    return full.reshape(CMP_BLOCK * n * HEAD_DIM, n * e)


def per_device(
    tokens,
    norm_gain,
    query_weight,
    cmp_key_weight,
    cmp_value_weight,
    sel_key_weight,
    sel_value_weight,
    branch_weight,
    key_embed,
    key_inner,
    key_outer,
    value_embed,
    value_inner,
    value_outer,
    out_weight,
    chosen,
):
    rows, width = tokens.shape
    kv_local = key_embed.shape[0]
    heads_local = query_weight.shape[1] // HEAD_DIM
    owners = lax.axis_size("kv")
    me = lax.axis_index("kv")
    planes = PLANES if owners % PLANES == 0 else 1
    across = owners // planes
    my_z, my_x = me // across, me % across
    offset = me * rows
    f32 = jnp.float32
    bf16 = jnp.bfloat16

    half = HEAD_DIM // 2
    lane = jnp.arange(LANES, dtype=jnp.int32)
    inverse = ROPE_BASE ** (-(lane % half).astype(f32) / half)
    positions = offset + jnp.arange(rows, dtype=jnp.int32)
    phases = positions.astype(f32)[:, None] * inverse[None, :]
    cosine = jnp.cos(phases)
    sine = jnp.sin(phases)
    first = (lane % HEAD_DIM < half)[None, :]
    up = jnp.where(first, -sine, 0.0)
    down = jnp.where(first, 0.0, sine)
    gain = norm_gain.reshape(1, width)

    def heads_of(w, k):
        return w[:, k * HEAD_DIM : (k + 1) * HEAD_DIM]

    sel_weight = jnp.concatenate(
        [heads_of(w, k) for k in range(kv_local) for w in (sel_key_weight, sel_value_weight)],
        axis=1,
    )
    tile = 256
    steps = rows // tile
    row_spec = lambda cols: pl.BlockSpec((tile, cols), lambda i: (i, 0))
    full = lambda shape: pl.BlockSpec(shape, lambda *_: (0,) * len(shape))
    kv = pl.pallas_call(
        sel_kernel,
        grid=(steps,),
        in_specs=[row_spec(width), full((1, width)), full(sel_weight.shape)]
        + [row_spec(LANES)] * 3,
        out_specs=[row_spec(LANES)] * kv_local,
        out_shape=[jax.ShapeDtypeStruct((rows, LANES), bf16)] * kv_local,
        compiler_params=params(1),
        cost_estimate=cost(2 * rows * width * sel_weight.shape[1], rows * width * 2),
        name="sel_project",
    )(tokens, gain, sel_weight, cosine, up, down)

    def hop(x, dz, dx):
        pairs = []
        for z in range(planes):
            for c in range(across):
                source, target = z * across + c, (z + dz) * across + (c + dx) % across
                if z + dz < planes:
                    pairs.append((source, target))
        return lax.ppermute(x, "kv", pairs)

    gate_cols = lax.dynamic_slice_in_dim(
        branch_weight, lax.axis_index("tp") * heads_local, heads_local, 2
    )
    gate_weight = jnp.concatenate([gate_cols[0], gate_cols[1]], axis=1)
    gate_count = 2 * heads_local
    mid_weight = jnp.concatenate(
        [query_weight, cmp_key_weight, cmp_value_weight, jnp.pad(gate_weight, ((0, 0), (0, LANES - gate_count)))],
        axis=1,
    )
    q_spec = pl.BlockSpec((kv_local, 2, tile, LANES), lambda i: (0, 0, i, 0))
    q_shape = jax.ShapeDtypeStruct((kv_local, 2, rows, LANES), bf16)
    kv_width = kv_local * HEAD_DIM
    q_plain, q_turn, cmp_key, cmp_value, gates = pl.pallas_call(
        mid_kernel,
        grid=(steps,),
        in_specs=[row_spec(width), full((1, width)), full(mid_weight.shape)]
        + [row_spec(LANES)] * 3,
        out_specs=[q_spec, q_spec, row_spec(kv_width), row_spec(kv_width), row_spec(LANES)],
        out_shape=[
            q_shape,
            q_shape,
            jax.ShapeDtypeStruct((rows, kv_width), f32),
            jax.ShapeDtypeStruct((rows, kv_width), f32),
            jax.ShapeDtypeStruct((rows, LANES), f32),
        ],
        compiler_params=params(1),
        cost_estimate=cost(2 * rows * width * mid_weight.shape[1], rows * width * 2),
        name="mid_project",
    )(tokens, gain, mid_weight, cosine, up, down)
    gates = gates[:, :gate_count]

    blocks = rows // CMP_BLOCK
    embeds = [
        e.astype(f32).transpose(1, 0, 2).reshape(CMP_BLOCK, kv_width)
        for e in (key_embed, value_embed)
    ]
    operands = (
        cmp_key,
        cmp_value,
        embeds[0],
        inner_diagonal(key_inner),
        block_diagonal(key_outer),
        embeds[1],
        inner_diagonal(value_inner),
        block_diagonal(value_outer),
    )
    summary = pl.pallas_call(
        summary_kernel,
        out_shape=jax.ShapeDtypeStruct((kv_local, blocks, LANES), bf16),
        in_specs=[pl.BlockSpec(memory_space=pltpu.VMEM)] * len(operands),
        out_specs=pl.BlockSpec(memory_space=pltpu.VMEM),
        compiler_params=pltpu.CompilerParams(vmem_limit_bytes=48 * 1024 * 1024),
        cost_estimate=cost(8e8, 4e6),
        name="summaries",
    )(*operands)

    moves = [(dz, dx) for dz in range(planes) for dx in range(across)]
    spans = []
    for dz, dx in moves:
        z, x = my_z - dz, (my_x - dx) % across
        span = z * across + x
        spans.append(jnp.where((z >= 0) & (span <= me), span, -1))
    spans = jnp.stack(spans)
    sums = [summary if move == (0, 0) else hop(summary, *move) for move in moves]
    starts = jnp.concatenate([offset[None], jnp.where(spans >= 0, spans * rows, -1)])
    starts = starts.astype(jnp.int32)

    far = [[None] * len(moves) for _ in range(kv_local)]
    for k in range(kv_local):
        column = [kv[k]]
        for dz in range(1, planes):
            column.append(hop(column[-1], 1, 0))
        for n, (dz, dx) in enumerate(moves):
            far[k][n] = column[dz] if dx == 0 else hop(column[dz], 0, dx)

    q_tile = pl.BlockSpec((kv_local, 2, tile, LANES), lambda i, s: (0, 0, i, 0))
    out_cmp = pl.pallas_call(
        cmp_kernel,
        grid_spec=pltpu.PrefetchScalarGridSpec(
            num_scalar_prefetch=1,
            grid=(steps,),
            in_specs=[q_tile, pl.BlockSpec((tile, gate_count), lambda i, s: (i, 0))]
            + [full(summary.shape)] * len(sums),
            out_specs=pl.BlockSpec((kv_local, tile, LANES), lambda i, s: (0, i, 0)),
        ),
        out_shape=jax.ShapeDtypeStruct((kv_local, rows, LANES), f32),
        compiler_params=params(1),
        cost_estimate=cost(1.5e10, 6e6),
        name="compressed",
    )(starts, q_plain, gates, *sums)

    q_blocks = rows // Q_BLOCK
    span_blocks = rows // SEL_BLOCK
    picks = lax.dynamic_slice_in_dim(chosen.astype(jnp.int32), me * q_blocks, q_blocks, 1)
    own_first = (me * q_blocks + jnp.arange(q_blocks, dtype=jnp.int32)) * (Q_BLOCK // SEL_BLOCK)
    usable = picks < own_first[None, :, None]
    hit = (picks[..., None, :] // span_blocks == spans[:, None]) & usable[..., None, :]
    inside = jnp.sum(jnp.where(hit, picks[..., None, :] % span_blocks, 0), axis=-1)
    bias = jnp.where(jnp.any(hit, axis=-1), 0.0, MASKED).astype(f32)
    bias = jnp.repeat(bias, SEL_BLOCK, axis=-1)
    bias = jnp.pad(bias, ((0, 0), (0, 0), (Q_BLOCK, 0)))[:, :, None, :]

    mixed = []
    for k in range(kv_local):
        mixed.append(
            pl.pallas_call(
                functools.partial(chosen_kernel, k),
                grid_spec=pltpu.PrefetchScalarGridSpec(
                    num_scalar_prefetch=1,
                    grid=(q_blocks,),
                    in_specs=[
                        pl.BlockSpec((1, 1, bias.shape[-1]), lambda j, s: (j, 0, 0)),
                        pl.BlockSpec((1, 2, Q_BLOCK, LANES), lambda j, s, k=k: (k, 0, j, 0)),
                        pl.BlockSpec((Q_BLOCK, gate_count), lambda j, s: (j, 0)),
                        pl.BlockSpec((1, Q_BLOCK, LANES), lambda j, s, k=k: (k, j, 0)),
                    ]
                    + [full((rows, LANES))] * len(moves),
                    out_specs=pl.BlockSpec((Q_BLOCK, LANES), lambda j, s: (j, 0)),
                ),
                out_shape=jax.ShapeDtypeStruct((rows, LANES), bf16),
                compiler_params=params(1),
                cost_estimate=cost(8e9, 6e6),
                name=f"chosen_{k}",
            )(inside[k].reshape(-1), bias[k], q_turn, gates, out_cmp, *far[k])
        )
    sent = [lax.all_to_all(m, "tp", split_axis=0, concat_axis=1, tiled=True) for m in mixed]
    ranks = lax.axis_size("tp")
    weight = out_weight.reshape(ranks, kv_local, LANES, -1)
    total = sum(
        jnp.dot(s, weight[:, k].reshape(ranks * LANES, -1), preferred_element_type=f32)
        for k, s in enumerate(sent)
    )
    return total.astype(bf16)


def solution(mesh):
    placed = (
        P("kv", None),
        P(),
        P(None, "tp"),
        P(None, "tp"),
        P(None, "tp"),
        P(None, "tp"),
        P(None, "tp"),
        P(),
        P("tp", None, None),
        P("tp", None, None),
        P("tp", None, None),
        P("tp", None, None),
        P("tp", None, None),
        P("tp", None, None),
        P(),
        P("tp", None, None),
    )
    return jax.shard_map(
        per_device, mesh=mesh, in_specs=placed, out_specs=P(("kv", "tp"), None), check_vma=False
    )
```

```python
import functools

import jax
import jax.numpy as jnp
from jax import lax
from jax.experimental import pallas as pl
from jax.experimental.pallas import tpu as pltpu
from jax.sharding import PartitionSpec as P

HEAD_DIM = 64
CMP_BLOCK = 32
SEL_BLOCK = 64
Q_BLOCK = 128
FAR_PICKS = 8
LANES = 2 * HEAD_DIM
PLANES = 4

ROPE_BASE = 10000.0
norm_eps = 1e-06
MASKED = -1e30


def params(n_axes, limit=48):
    return pltpu.CompilerParams(
        dimension_semantics=("arbitrary",) * n_axes, vmem_limit_bytes=limit * 1024 * 1024
    )


def norm_rows(tok_ref, gain_ref):
    x = tok_ref[...].astype(jnp.float32)
    inv = lax.rsqrt(jnp.mean(x * x, axis=-1, keepdims=True) + norm_eps)
    return (x * inv * gain_ref[...].astype(jnp.float32)).astype(jnp.bfloat16)


def turn(x, cosine, sine_up, sine_down):
    quarter = HEAD_DIM // 2
    return (
        x * cosine
        + pltpu.roll(x, LANES - quarter, 1) * sine_up
        + pltpu.roll(x, quarter, 1) * sine_down
    )


def low_lanes(shape):
    return lax.broadcasted_iota(jnp.int32, shape, 1) < HEAD_DIM


def sel_kernel(tok_ref, gain_ref, w_ref, cos_ref, up_ref, down_ref, *outs):
    normed = norm_rows(tok_ref, gain_ref)
    y = jnp.dot(normed, w_ref[...], preferred_element_type=jnp.float32)
    for k, out in enumerate(outs):
        x = y[:, k * LANES : (k + 1) * LANES]
        low = low_lanes(x.shape)
        turned = turn(x, cos_ref[...], up_ref[...], down_ref[...])
        out[...] = jnp.where(low, turned, x).astype(jnp.bfloat16)


def mid_kernel(
    tok_ref,
    gain_ref,
    w_ref,
    cos_ref,
    up_ref,
    down_ref,
    qp_ref,
    qt_ref,
    ck_ref,
    cv_ref,
    gate_ref,
):
    scale = HEAD_DIM ** (-0.5)
    normed = norm_rows(tok_ref, gain_ref)
    y = jnp.dot(normed, w_ref[...], preferred_element_type=jnp.float32)
    kv_local = qp_ref.shape[0]
    for k in range(kv_local):
        x = y[:, k * LANES : (k + 1) * LANES]
        low = low_lanes(x.shape)
        turned = turn(x, cos_ref[...], up_ref[...], down_ref[...]) * scale
        plain = x * scale
        for ref, v in ((qp_ref, plain), (qt_ref, turned)):
            ref[k, 0] = jnp.where(low, v, 0.0).astype(jnp.bfloat16)
            ref[k, 1] = jnp.where(low, pltpu.roll(v, HEAD_DIM, 1), 0.0).astype(jnp.bfloat16)
    base = kv_local * LANES
    width = kv_local * HEAD_DIM
    ck_ref[...] = y[:, base : base + width].astype(jnp.bfloat16).astype(jnp.float32)
    cv_ref[...] = y[:, base + width : base + 2 * width].astype(jnp.bfloat16).astype(jnp.float32)
    gate_ref[...] = jax.nn.sigmoid(y[:, base + 2 * width :])


def summary_kernel(ck_ref, cv_ref, ke_ref, ki_ref, ko_ref, ve_ref, vi_ref, vo_ref, out_ref):
    blocks = ck_ref.shape[0] // CMP_BLOCK

    def one(x_ref, e_ref, i_ref, o_ref):
        rows = []
        for c in range(CMP_BLOCK):
            part = x_ref[pl.ds(c, blocks, stride=CMP_BLOCK), :] + e_ref[c : c + 1, :]
            rows.append(part.astype(jnp.bfloat16))
        flat = jnp.concatenate(rows, axis=1)
        hidden = jnp.dot(flat, i_ref[...], preferred_element_type=jnp.float32)
        hidden = jax.nn.gelu(hidden).astype(jnp.bfloat16)
        return jnp.dot(hidden, o_ref[...], preferred_element_type=jnp.float32)

    sk = one(ck_ref, ke_ref, ki_ref, ko_ref)
    sv = one(cv_ref, ve_ref, vi_ref, vo_ref)
    for k in range(out_ref.shape[0]):
        at = slice(k * HEAD_DIM, (k + 1) * HEAD_DIM)
        out_ref[k] = jnp.concatenate([sk[:, at], sv[:, at]], axis=1).astype(jnp.bfloat16)


def nt_dot(a, b):
    return lax.dot_general(a, b, (((1,), (1,)), ((), ())), preferred_element_type=jnp.float32)


def gate_lanes(gate, first, shape):
    return jnp.where(low_lanes(shape), gate[:, first : first + 1], gate[:, first + 1 : first + 2])


def merge(out, rows):
    low = low_lanes((rows, LANES))
    return jnp.where(low, pltpu.roll(out[:rows], HEAD_DIM, 1), out[rows:])


def cmp_kernel(start_ref, q_ref, gate_ref, *rest):
    sums, out_ref = rest[:-1], rest[-1]
    rows = q_ref.shape[2]
    per = sums[0].shape[1]
    start = start_ref[0]
    tile_at = pl.program_id(0) * rows
    kv_local = q_ref.shape[0]
    lane = lax.broadcasted_iota(jnp.int32, (1, per * len(sums)), 1)
    ends = jnp.zeros_like(lane)
    for a in range(len(sums)):
        first = start_ref[a + 1]
        local = (lane - a * per + 1) * CMP_BLOCK - 1 + first
        local = jnp.where(first < 0, jnp.int32(2**30), local)
        ends = jnp.where((lane >= a * per) & (lane < (a + 1) * per), local, ends)
    row = lax.broadcasted_iota(jnp.int32, (2 * rows, 1), 0)
    pos = start + tile_at + jnp.where(row >= rows, row - rows, row)
    allowed = ends <= pos
    for k in range(kv_local):
        keys = jnp.concatenate([s[k] for s in sums], axis=0)
        q = jnp.concatenate([q_ref[k, 0], q_ref[k, 1]], axis=0)
        s = jnp.where(allowed, nt_dot(q, keys), MASKED)
        top = jnp.max(s, axis=-1, keepdims=True)
        e = jnp.where(allowed, jnp.exp(s - top), 0.0)
        total = jnp.sum(e, axis=-1, keepdims=True)
        o = jnp.dot(e.astype(jnp.bfloat16), keys, preferred_element_type=jnp.float32)
        o = o * jnp.where(total > 0.0, 1.0 / jnp.where(total > 0.0, total, 1.0), 0.0)
        o = merge(o, rows)
        g = gate_lanes(gate_ref[...], 2 * k, o.shape)
        out_ref[k] = o * g


def chosen_kernel(head, idx_ref, bias_ref, q_ref, gate_ref, oc_ref, *rest):
    stores, out_ref = rest[:-1], rest[-1]
    count = bias_ref.shape[0]
    base = pl.program_id(0) * count
    for u in range(count):
        j = base + u
        at_rows = slice(u * Q_BLOCK, (u + 1) * Q_BLOCK)
        parts = [stores[0][pl.ds(pl.multiple_of(j * Q_BLOCK, Q_BLOCK), Q_BLOCK), :]]
        for a, store in enumerate(stores):
            at = pl.multiple_of(idx_ref[j * len(stores) + a] * SEL_BLOCK, SEL_BLOCK)
            parts.append(store[pl.ds(at, SEL_BLOCK), :])
        keys = jnp.concatenate(parts, axis=0)
        q = jnp.concatenate([q_ref[0, 0, at_rows], q_ref[0, 1, at_rows]], axis=0)
        s = nt_dot(q, keys) + bias_ref[u]
        row = lax.broadcasted_iota(jnp.int32, (2 * Q_BLOCK, Q_BLOCK), 0)
        row = jnp.where(row >= Q_BLOCK, row - Q_BLOCK, row)
        lane = lax.broadcasted_iota(jnp.int32, row.shape, 1)
        near = jnp.where(lane > row, MASKED, s[:, :Q_BLOCK])
        s = jnp.concatenate([near, s[:, Q_BLOCK:]], axis=1)
        top = jnp.max(s, axis=-1, keepdims=True)
        e = jnp.exp(s - top)
        total = jnp.sum(e, axis=-1, keepdims=True)
        o = jnp.dot(e.astype(jnp.bfloat16), keys, preferred_element_type=jnp.float32)
        o = merge(o * (1.0 / total), Q_BLOCK)
        gate = gate_ref[at_rows]
        g = gate_lanes(gate, gate.shape[1] // 2 + 2 * head, o.shape)
        out_ref[at_rows] = (oc_ref[0, at_rows] + o * g).astype(jnp.bfloat16)


def cost(flops, moved):
    return pl.CostEstimate(flops=int(flops), bytes_accessed=int(moved), transcendentals=0)


def block_diagonal(w):
    n, a, b = w.shape
    zero = jnp.zeros((a, b), w.dtype)
    return jnp.concatenate(
        [jnp.concatenate([w[i] if i == j else zero for j in range(n)], axis=1) for i in range(n)],
        axis=0,
    )


def inner_diagonal(w):
    n, rows, e = w.shape
    w = w.reshape(n, CMP_BLOCK, HEAD_DIM, e)
    zero = jnp.zeros_like(w[0])
    full = jnp.stack(
        [jnp.concatenate([w[i] if i == j else zero for j in range(n)], axis=-1) for i in range(n)],
        axis=1,
    )
    return full.reshape(CMP_BLOCK * n * HEAD_DIM, n * e)


def per_device(
    tokens,
    norm_gain,
    query_weight,
    cmp_key_weight,
    cmp_value_weight,
    sel_key_weight,
    sel_value_weight,
    branch_weight,
    key_embed,
    key_inner,
    key_outer,
    value_embed,
    value_inner,
    value_outer,
    out_weight,
    chosen,
):
    rows, width = tokens.shape
    kv_local = key_embed.shape[0]
    heads_local = query_weight.shape[1] // HEAD_DIM
    owners = lax.axis_size("kv")
    me = lax.axis_index("kv")
    planes = PLANES if owners % PLANES == 0 else 1
    across = owners // planes
    my_z, my_x = me // across, me % across
    offset = me * rows
    f32 = jnp.float32
    bf16 = jnp.bfloat16

    half = HEAD_DIM // 2
    lane = jnp.arange(LANES, dtype=jnp.int32)
    inverse = ROPE_BASE ** (-(lane % half).astype(f32) / half)
    positions = offset + jnp.arange(rows, dtype=jnp.int32)
    phases = positions.astype(f32)[:, None] * inverse[None, :]
    cosine = jnp.cos(phases)
    sine = jnp.sin(phases)
    first = (lane % HEAD_DIM < half)[None, :]
    up = jnp.where(first, -sine, 0.0)
    down = jnp.where(first, 0.0, sine)
    gain = norm_gain.reshape(1, width)

    def heads_of(w, k):
        return w[:, k * HEAD_DIM : (k + 1) * HEAD_DIM]

    sel_weight = jnp.concatenate(
        [heads_of(w, k) for k in range(kv_local) for w in (sel_key_weight, sel_value_weight)],
        axis=1,
    )
    tile = 256
    steps = rows // tile
    row_spec = lambda cols: pl.BlockSpec((tile, cols), lambda i: (i, 0))
    full = lambda shape: pl.BlockSpec(shape, lambda *_: (0,) * len(shape))
    kv = pl.pallas_call(
        sel_kernel,
        grid=(steps,),
        in_specs=[row_spec(width), full((1, width)), full(sel_weight.shape)]
        + [row_spec(LANES)] * 3,
        out_specs=[row_spec(LANES)] * kv_local,
        out_shape=[jax.ShapeDtypeStruct((rows, LANES), bf16)] * kv_local,
        compiler_params=params(1),
        cost_estimate=cost(2 * rows * width * sel_weight.shape[1], rows * width * 2),
        name="sel_project",
    )(tokens, gain, sel_weight, cosine, up, down)

    def hop(x, dz, dx):
        pairs = []
        for z in range(planes):
            for c in range(across):
                source, target = z * across + c, (z + dz) * across + (c + dx) % across
                if z + dz < planes:
                    pairs.append((source, target))
        return lax.ppermute(x, "kv", pairs)

    later, kv = lax.optimization_barrier((tokens, kv))
    gate_cols = lax.dynamic_slice_in_dim(
        branch_weight, lax.axis_index("tp") * heads_local, heads_local, 2
    )
    gate_weight = jnp.concatenate([gate_cols[0], gate_cols[1]], axis=1)
    gate_count = 2 * heads_local
    mid_weight = jnp.concatenate(
        [query_weight, cmp_key_weight, cmp_value_weight, jnp.pad(gate_weight, ((0, 0), (0, LANES - gate_count)))],
        axis=1,
    )
    q_spec = pl.BlockSpec((kv_local, 2, tile, LANES), lambda i: (0, 0, i, 0))
    q_shape = jax.ShapeDtypeStruct((kv_local, 2, rows, LANES), bf16)
    kv_width = kv_local * HEAD_DIM
    q_plain, q_turn, cmp_key, cmp_value, gates = pl.pallas_call(
        mid_kernel,
        grid=(steps,),
        in_specs=[row_spec(width), full((1, width)), full(mid_weight.shape)]
        + [row_spec(LANES)] * 3,
        out_specs=[q_spec, q_spec, row_spec(kv_width), row_spec(kv_width), row_spec(LANES)],
        out_shape=[
            q_shape,
            q_shape,
            jax.ShapeDtypeStruct((rows, kv_width), f32),
            jax.ShapeDtypeStruct((rows, kv_width), f32),
            jax.ShapeDtypeStruct((rows, LANES), f32),
        ],
        compiler_params=params(1),
        cost_estimate=cost(2 * rows * width * mid_weight.shape[1], rows * width * 2),
        name="mid_project",
    )(later, gain, mid_weight, cosine, up, down)
    gates = gates[:, :gate_count]

    blocks = rows // CMP_BLOCK
    embeds = [
        e.astype(f32).transpose(1, 0, 2).reshape(CMP_BLOCK, kv_width)
        for e in (key_embed, value_embed)
    ]
    operands = (
        cmp_key,
        cmp_value,
        embeds[0],
        inner_diagonal(key_inner),
        block_diagonal(key_outer),
        embeds[1],
        inner_diagonal(value_inner),
        block_diagonal(value_outer),
    )
    summary = pl.pallas_call(
        summary_kernel,
        out_shape=jax.ShapeDtypeStruct((kv_local, blocks, LANES), bf16),
        in_specs=[pl.BlockSpec(memory_space=pltpu.VMEM)] * len(operands),
        out_specs=pl.BlockSpec(memory_space=pltpu.VMEM),
        compiler_params=pltpu.CompilerParams(vmem_limit_bytes=48 * 1024 * 1024),
        cost_estimate=cost(8e8, 4e6),
        name="summaries",
    )(*operands)

    moves = [(dz, dx) for dz in range(planes) for dx in range(across)]
    spans = []
    for dz, dx in moves:
        z, x = my_z - dz, (my_x - dx) % across
        span = z * across + x
        spans.append(jnp.where((z >= 0) & (span <= me), span, -1))
    spans = jnp.stack(spans)
    sums = [summary if move == (0, 0) else hop(summary, *move) for move in moves]
    starts = jnp.concatenate([offset[None], jnp.where(spans >= 0, spans * rows, -1)])
    starts = starts.astype(jnp.int32)

    far = [[None] * len(moves) for _ in range(kv_local)]
    for k in range(kv_local):
        column = [kv[k]]
        for dz in range(1, planes):
            column.append(hop(column[-1], 1, 0))
        for n, (dz, dx) in enumerate(moves):
            far[k][n] = column[dz] if dx == 0 else hop(column[dz], 0, dx)

    q_tile = pl.BlockSpec((kv_local, 2, tile, LANES), lambda i, s: (0, 0, i, 0))
    out_cmp = pl.pallas_call(
        cmp_kernel,
        grid_spec=pltpu.PrefetchScalarGridSpec(
            num_scalar_prefetch=1,
            grid=(steps,),
            in_specs=[q_tile, pl.BlockSpec((tile, gate_count), lambda i, s: (i, 0))]
            + [full(summary.shape)] * len(sums),
            out_specs=pl.BlockSpec((kv_local, tile, LANES), lambda i, s: (0, i, 0)),
        ),
        out_shape=jax.ShapeDtypeStruct((kv_local, rows, LANES), f32),
        compiler_params=params(1),
        cost_estimate=cost(1.5e10, 6e6),
        name="compressed",
    )(starts, q_plain, gates, *sums)

    q_blocks = rows // Q_BLOCK
    span_blocks = rows // SEL_BLOCK
    picks = lax.dynamic_slice_in_dim(chosen.astype(jnp.int32), me * q_blocks, q_blocks, 1)
    own_first = (me * q_blocks + jnp.arange(q_blocks, dtype=jnp.int32)) * (Q_BLOCK // SEL_BLOCK)
    usable = picks < own_first[None, :, None]
    hit = (picks[..., None, :] // span_blocks == spans[:, None]) & usable[..., None, :]
    inside = jnp.sum(jnp.where(hit, picks[..., None, :] % span_blocks, 0), axis=-1)
    bias = jnp.where(jnp.any(hit, axis=-1), 0.0, MASKED).astype(f32)
    bias = jnp.repeat(bias, SEL_BLOCK, axis=-1)
    bias = jnp.pad(bias, ((0, 0), (0, 0), (Q_BLOCK, 0)))[:, :, None, :]

    mixed = []
    group = 4
    g_rows = group * Q_BLOCK
    for k in range(kv_local):
        mixed.append(
            pl.pallas_call(
                functools.partial(chosen_kernel, k),
                grid_spec=pltpu.PrefetchScalarGridSpec(
                    num_scalar_prefetch=1,
                    grid=(q_blocks // group,),
                    in_specs=[
                        pl.BlockSpec((group, 1, bias.shape[-1]), lambda j, s: (j, 0, 0)),
                        pl.BlockSpec((1, 2, g_rows, LANES), lambda j, s, k=k: (k, 0, j, 0)),
                        pl.BlockSpec((g_rows, gate_count), lambda j, s: (j, 0)),
                        pl.BlockSpec((1, g_rows, LANES), lambda j, s, k=k: (k, j, 0)),
                    ]
                    + [full((rows, LANES))] * len(moves),
                    out_specs=pl.BlockSpec((g_rows, LANES), lambda j, s: (j, 0)),
                ),
                out_shape=jax.ShapeDtypeStruct((rows, LANES), bf16),
                compiler_params=params(1),
                cost_estimate=cost(8e9, 6e6),
                name=f"chosen_{k}",
            )(inside[k].reshape(-1), bias[k], q_turn, gates, out_cmp, *far[k])
        )
    sent = [lax.all_to_all(m, "tp", split_axis=0, concat_axis=1, tiled=True) for m in mixed]
    ranks = lax.axis_size("tp")
    weight = out_weight.reshape(ranks, kv_local, LANES, -1)
    total = sum(
        jnp.dot(s, weight[:, k].reshape(ranks * LANES, -1), preferred_element_type=f32)
        for k, s in enumerate(sent)
    )
    return total.astype(bf16)


def solution(mesh):
    placed = (
        P("kv", None),
        P(),
        P(None, "tp"),
        P(None, "tp"),
        P(None, "tp"),
        P(None, "tp"),
        P(None, "tp"),
        P(),
        P("tp", None, None),
        P("tp", None, None),
        P("tp", None, None),
        P("tp", None, None),
        P("tp", None, None),
        P("tp", None, None),
        P(),
        P("tp", None, None),
    )
    return jax.shard_map(
        per_device, mesh=mesh, in_specs=placed, out_specs=P(("kv", "tp"), None), check_vma=False
    )
```

```python
import functools

import jax
import jax.numpy as jnp
from jax import lax
from jax.experimental import pallas as pl
from jax.experimental.pallas import tpu as pltpu
from jax.sharding import PartitionSpec as P

HEAD_DIM = 64
CMP_BLOCK = 32
SEL_BLOCK = 64
Q_BLOCK = 128
FAR_PICKS = 8
LANES = 2 * HEAD_DIM
PLANES = 4
MESH = pl.DeviceIdType.MESH

ROPE_BASE = 10000.0
norm_eps = 1e-06
MASKED = -1e30

def params(n_axes, limit=48):
    return pltpu.CompilerParams(
        dimension_semantics=("arbitrary",) * n_axes, vmem_limit_bytes=limit * 1024 * 1024
    )


def norm_rows(tok_ref, gain_ref):
    x = tok_ref[...].astype(jnp.float32)
    inv = lax.rsqrt(jnp.mean(x * x, axis=-1, keepdims=True) + norm_eps)
    return (x * inv * gain_ref[...].astype(jnp.float32)).astype(jnp.bfloat16)


def turn(x, cosine, sine_up, sine_down):
    quarter = HEAD_DIM // 2
    return (
        x * cosine
        + pltpu.roll(x, LANES - quarter, 1) * sine_up
        + pltpu.roll(x, quarter, 1) * sine_down
    )


def low_lanes(shape):
    return lax.broadcasted_iota(jnp.int32, shape, 1) < HEAD_DIM


def sel_kernel(tok_ref, gain_ref, w_ref, cos_ref, up_ref, down_ref, *outs):
    normed = norm_rows(tok_ref, gain_ref)
    y = jnp.dot(normed, w_ref[...], preferred_element_type=jnp.float32)
    for k, out in enumerate(outs):
        x = y[:, k * LANES : (k + 1) * LANES]
        low = low_lanes(x.shape)
        turned = turn(x, cos_ref[...], up_ref[...], down_ref[...])
        out[...] = jnp.where(low, turned, x).astype(jnp.bfloat16)


def nt_dot(a, b):
    return lax.dot_general(a, b, (((1,), (1,)), ((), ())), preferred_element_type=jnp.float32)


def gate_lanes(gate, first, shape):
    return jnp.where(low_lanes(shape), gate[:, first : first + 1], gate[:, first + 1 : first + 2])


def merge(out, rows):
    low = low_lanes((rows, LANES))
    return jnp.where(low, pltpu.roll(out[:rows], HEAD_DIM, 1), out[rows:])


def exchange_kernel(
    planes,
    idx_ref,
    bias_ref,
    gain_ref,
    ke_ref,
    ko_ref,
    ve_ref,
    vo_ref,
    tok_hbm,
    w_hbm,
    cos_hbm,
    up_hbm,
    down_hbm,
    ki_hbm,
    vi_hbm,
    *rest,
):
    kv_local = bias_ref.shape[0]
    own_hbm, rest = rest[:kv_local], rest[kv_local:]
    out_ref, rest = rest[0], rest[1:]
    held, rest = rest[:kv_local], rest[kv_local:]
    (
        tok,
        w,
        cosine,
        up,
        down,
        ki,
        vi,
        qp,
        qt,
        ck,
        cv,
        gate,
        sums,
        oc,
        mix,
        got,
        local_sem,
        send_sem,
        recv_sem,
        sum_send,
        sum_recv,
        mix_send,
        mix_recv,
    ) = rest
    owners, ranks = sums.shape[0], got.shape[0]
    rows, width = tok.shape
    span = rows // SEL_BLOCK
    across = owners // planes
    me, rank = lax.axis_index("kv"), lax.axis_index("tp")
    z, x = me // across, me % across

    barrier = pltpu.get_barrier_semaphore()
    for d in range(1, owners):
        pl.semaphore_signal(barrier, inc=1, device_id={"kv": (me + d) % owners}, device_id_type=MESH)
    for d in range(1, ranks):
        pl.semaphore_signal(barrier, inc=1, device_id={"tp": (rank + d) % ranks}, device_id_type=MESH)
    loads = [
        (tok_hbm, tok),
        (w_hbm, w),
        (cos_hbm, cosine),
        (up_hbm, up),
        (down_hbm, down),
        (ki_hbm, ki),
        (vi_hbm, vi),
    ]
    copies = [pltpu.make_async_copy(a, b, local_sem.at[n]) for n, (a, b) in enumerate(loads)]
    for k in range(kv_local):
        copies.append(
            pltpu.make_async_copy(own_hbm[k], held[k].at[pl.ds(0, span)], local_sem.at[len(loads) + k])
        )
    for copy in copies:
        copy.start()
    pl.semaphore_wait(barrier, owners + ranks - 2)

    def slot(k, n):
        return held[k].at[pl.ds(n * span, span)]

    def hop(k, dz, dx):
        n = dz * across + dx
        if dx:
            source = own_hbm[k] if dz == 0 else slot(k, dz * across)
            target = z * across + (x + dx) % across
            sends = (x + dx < across) if dz == 0 else (z >= dz)
            gets = (x >= dx) if dz == 0 else (z >= dz)
        else:
            step = 1 if dz == 3 else dz
            source = slot(k, 2 * across) if dz == 3 else own_hbm[k]
            target = lax.rem(me + step * across, owners)
            sends = (z == 2) if dz == 3 else (z + dz < planes)
            gets = z >= dz
        copy = pltpu.make_async_remote_copy(
            src_ref=source,
            dst_ref=slot(k, n),
            send_sem=send_sem.at[k, n],
            recv_sem=recv_sem.at[k, n],
            device_id={"kv": target},
            device_id_type=MESH,
        )
        return copy, sends, gets

    def send(k, dz, dx):
        copy, sends, _ = hop(k, dz, dx)
        pl.when(sends)(copy.start)

    def arrive(k, dz, dx):
        copy, _, gets = hop(k, dz, dx)
        pl.when(gets)(copy.wait_recv)

    def send_own(k):
        for dz in (2, 1):
            if dz < planes:
                send(k, dz, 0)
        for dx in range(1, across):
            send(k, 0, dx)

    def forward(k, dz):
        if dz >= planes:
            return
        arrive(k, dz, 0)
        if dz == 2 and planes > 3:
            send(k, 3, 0)
        for dx in range(1, across):
            send(k, dz, dx)

    send_own(0)
    for copy in copies:
        copy.wait()

    tile = 256
    scale = HEAD_DIM ** (-0.5)
    base = kv_local * LANES
    kv_width = kv_local * HEAD_DIM

    def project(i, carry):
        at = pl.ds(pl.multiple_of(i * tile, tile), tile)
        normed = norm_rows(tok.at[at], gain_ref)
        y = jnp.dot(normed, w[...], preferred_element_type=jnp.float32)
        for k in range(kv_local):
            v = y[:, k * LANES : (k + 1) * LANES]
            low = low_lanes(v.shape)
            turned = turn(v, cosine[at], up[at], down[at]) * scale
            for ref, q in ((qp, v * scale), (qt, turned)):
                ref[k, 0, at] = jnp.where(low, q, 0.0).astype(jnp.bfloat16)
                ref[k, 1, at] = jnp.where(low, pltpu.roll(q, HEAD_DIM, 1), 0.0).astype(jnp.bfloat16)
        ck[at] = y[:, base : base + kv_width].astype(jnp.bfloat16).astype(jnp.float32)
        cv[at] = y[:, base + kv_width : base + 2 * kv_width].astype(jnp.bfloat16).astype(jnp.float32)
        gate[at] = jax.nn.sigmoid(y[:, base + 2 * kv_width :])
        return carry

    lax.fori_loop(0, rows // tile, project, 0)

    blocks = rows // CMP_BLOCK

    def summarize(x_ref, e_ref, i_ref, o_ref):
        parts = []
        for c in range(CMP_BLOCK):
            part = x_ref[pl.ds(c, blocks, stride=CMP_BLOCK), :] + e_ref[c : c + 1, :]
            parts.append(part.astype(jnp.bfloat16))
        flat = jnp.concatenate(parts, axis=1)
        hidden = jnp.dot(flat, i_ref[...], preferred_element_type=jnp.float32)
        hidden = jax.nn.gelu(hidden).astype(jnp.bfloat16)
        return jnp.dot(hidden, o_ref[...], preferred_element_type=jnp.float32)

    sk = summarize(ck, ke_ref, ki, ko_ref)
    sv = summarize(cv, ve_ref, vi, vo_ref)
    for k in range(kv_local):
        cut = slice(k * HEAD_DIM, (k + 1) * HEAD_DIM)
        sums[me, k] = jnp.concatenate([sk[:, cut], sv[:, cut]], axis=1).astype(jnp.bfloat16)

    def sum_copy(d, source):
        return pltpu.make_async_remote_copy(
            src_ref=sums.at[source],
            dst_ref=sums.at[source],
            send_sem=sum_send.at[d],
            recv_sem=sum_recv.at[d],
            device_id={"kv": (me + d) % owners},
            device_id_type=MESH,
        )

    for d in range(1, owners):
        sum_copy(d, me).start()
    for k in range(1, kv_local):
        send_own(k)
    forward(0, 2)
    forward(0, 1)
    for d in range(1, owners):
        sum_copy(d, (me + owners - d) % owners).wait_recv()

    def compress(i, carry):
        at = pl.ds(pl.multiple_of(i * tile, tile), tile)
        row = lax.broadcasted_iota(jnp.int32, (2 * tile, 1), 0)
        pos = me * rows + i * tile + jnp.where(row >= tile, row - tile, row)
        lane = lax.broadcasted_iota(jnp.int32, (1, owners * blocks), 1)
        allowed = (lane + 1) * CMP_BLOCK - 1 <= pos
        for k in range(kv_local):
            keys = jnp.concatenate([sums[s, k] for s in range(owners)], axis=0)
            q = jnp.concatenate([qp[k, 0, at], qp[k, 1, at]], axis=0)
            s = jnp.where(allowed, nt_dot(q, keys), MASKED)
            top = jnp.max(s, axis=-1, keepdims=True)
            e = jnp.where(allowed, jnp.exp(s - top), 0.0)
            total = jnp.sum(e, axis=-1, keepdims=True)
            o = jnp.dot(e.astype(jnp.bfloat16), keys, preferred_element_type=jnp.float32)
            o = o * jnp.where(total > 0.0, 1.0 / jnp.where(total > 0.0, total, 1.0), 0.0)
            o = merge(o, tile)
            oc[k, at] = o * gate_lanes(gate[at], 2 * k, o.shape)
        return carry

    lax.fori_loop(0, rows // tile, compress, 0)

    rank_rows = rows // ranks
    group = rank_rows // Q_BLOCK
    q_blocks = rows // Q_BLOCK
    half_gates = 2 * kv_local

    def mix_copy(k, step):
        target = (rank + 1 + step) % ranks
        at = pl.ds(pl.multiple_of(target * rank_rows, rank_rows), rank_rows)
        return pltpu.make_async_remote_copy(
            src_ref=mix.at[k, at],
            dst_ref=got.at[rank, k],
            send_sem=mix_send.at[k, step],
            recv_sem=mix_recv.at[k, step],
            device_id={"tp": target},
            device_id_type=MESH,
        )

    def choose(k):
        def one(step, carry):
            target = (rank + 1 + step) % ranks
            for u in range(group):
                j = target * group + u
                at = pl.ds(pl.multiple_of(j * Q_BLOCK, Q_BLOCK), Q_BLOCK)
                own = j * (Q_BLOCK // SEL_BLOCK)
                parts = [held[k][own + b] for b in range(Q_BLOCK // SEL_BLOCK)]
                for a in range(FAR_PICKS):
                    pick = idx_ref[(k * q_blocks + j) * FAR_PICKS + a]
                    parts.append(held[k][pick])
                keys = jnp.concatenate(parts, axis=0)
                q = jnp.concatenate([qt[k, 0, at], qt[k, 1, at]], axis=0)
                s = nt_dot(q, keys) + bias_ref[k, j]
                row = lax.broadcasted_iota(jnp.int32, (2 * Q_BLOCK, Q_BLOCK), 0)
                row = jnp.where(row >= Q_BLOCK, row - Q_BLOCK, row)
                lane = lax.broadcasted_iota(jnp.int32, row.shape, 1)
                near = jnp.where(lane > row, MASKED, s[:, :Q_BLOCK])
                s = jnp.concatenate([near, s[:, Q_BLOCK:]], axis=1)
                top = jnp.max(s, axis=-1, keepdims=True)
                e = jnp.exp(s - top)
                total = jnp.sum(e, axis=-1, keepdims=True)
                o = jnp.dot(e.astype(jnp.bfloat16), keys, preferred_element_type=jnp.float32)
                o = merge(o * (1.0 / total), Q_BLOCK)
                g = gate_lanes(gate[at], half_gates + 2 * k, o.shape)
                mix[k, at] = (oc[k, at] + o * g).astype(jnp.bfloat16)
            pl.when(step > 0)(lambda: mix_copy(k, step - 1).start())
            return carry

        lax.fori_loop(0, ranks, one, 0)

    moves = [(dz, dx) for dz in range(planes) for dx in range(across) if (dz, dx) != (0, 0)]
    for k in range(kv_local):
        if k:
            forward(k, 2)
            forward(k, 1)
        forward(k, 3)
        for dz, dx in moves:
            if dx:
                arrive(k, dz, dx)
        choose(k)
    own_at = pl.ds(pl.multiple_of(rank * rank_rows, rank_rows), rank_rows)
    for k in range(kv_local):
        for dz, dx in moves:
            copy, sends, _ = hop(k, dz, dx)
            pl.when(sends)(copy.wait_send)
    for d in range(1, owners):
        sum_copy(d, me).wait_send()
    for k in range(kv_local):
        got[rank, k] = mix[k, own_at]
        for step in range(ranks - 1):
            mix_copy(k, step).wait_send()
            mix_copy(k, step).wait_recv()
    for t in range(ranks):
        for k in range(kv_local):
            first = (t * kv_local + k) * LANES
            out_ref[:, first : first + LANES] = got[t, k]


def cost(flops, moved):
    return pl.CostEstimate(flops=int(flops), bytes_accessed=int(moved), transcendentals=0)


def block_diagonal(w):
    n, a, b = w.shape
    zero = jnp.zeros((a, b), w.dtype)
    return jnp.concatenate(
        [jnp.concatenate([w[i] if i == j else zero for j in range(n)], axis=1) for i in range(n)],
        axis=0,
    )


def inner_diagonal(w):
    n, rows, e = w.shape
    w = w.reshape(n, CMP_BLOCK, HEAD_DIM, e)
    zero = jnp.zeros_like(w[0])
    full = jnp.stack(
        [jnp.concatenate([w[i] if i == j else zero for j in range(n)], axis=-1) for i in range(n)],
        axis=1,
    )
    return full.reshape(CMP_BLOCK * n * HEAD_DIM, n * e)


def per_device(
    tokens,
    norm_gain,
    query_weight,
    cmp_key_weight,
    cmp_value_weight,
    sel_key_weight,
    sel_value_weight,
    branch_weight,
    key_embed,
    key_inner,
    key_outer,
    value_embed,
    value_inner,
    value_outer,
    out_weight,
    chosen,
):
    rows, width = tokens.shape
    kv_local = key_embed.shape[0]
    heads_local = query_weight.shape[1] // HEAD_DIM
    owners = lax.axis_size("kv")
    me = lax.axis_index("kv")
    planes = PLANES if owners % PLANES == 0 else 1
    across = owners // planes
    my_z, my_x = me // across, me % across
    offset = me * rows
    f32 = jnp.float32
    bf16 = jnp.bfloat16

    half = HEAD_DIM // 2
    lane = jnp.arange(LANES, dtype=jnp.int32)
    inverse = ROPE_BASE ** (-(lane % half).astype(f32) / half)
    positions = offset + jnp.arange(rows, dtype=jnp.int32)
    phases = positions.astype(f32)[:, None] * inverse[None, :]
    cosine = jnp.cos(phases)
    sine = jnp.sin(phases)
    first = (lane % HEAD_DIM < half)[None, :]
    up = jnp.where(first, -sine, 0.0)
    down = jnp.where(first, 0.0, sine)
    gain = norm_gain.reshape(1, width)

    def heads_of(w, k):
        return w[:, k * HEAD_DIM : (k + 1) * HEAD_DIM]

    sel_weight = jnp.concatenate(
        [heads_of(w, k) for k in range(kv_local) for w in (sel_key_weight, sel_value_weight)],
        axis=1,
    )
    tile = 256
    steps = rows // tile
    row_spec = lambda cols: pl.BlockSpec((tile, cols), lambda i: (i, 0))
    full = lambda shape: pl.BlockSpec(shape, lambda *_: (0,) * len(shape))
    kv = pl.pallas_call(
        sel_kernel,
        grid=(steps,),
        in_specs=[row_spec(width), full((1, width)), full(sel_weight.shape)]
        + [row_spec(LANES)] * 3,
        out_specs=[row_spec(LANES)] * kv_local,
        out_shape=[jax.ShapeDtypeStruct((rows, LANES), bf16)] * kv_local,
        compiler_params=params(1),
        cost_estimate=cost(2 * rows * width * sel_weight.shape[1], rows * width * 2),
        name="sel_project",
    )(tokens, gain, sel_weight, cosine, up, down)

    gate_cols = lax.dynamic_slice_in_dim(
        branch_weight, lax.axis_index("tp") * heads_local, heads_local, 2
    )
    gate_weight = jnp.concatenate([gate_cols[0], gate_cols[1]], axis=1)
    gate_count = 2 * heads_local
    mid_weight = jnp.concatenate(
        [query_weight, cmp_key_weight, cmp_value_weight, jnp.pad(gate_weight, ((0, 0), (0, LANES - gate_count)))],
        axis=1,
    )
    kv_width = kv_local * HEAD_DIM
    blocks = rows // CMP_BLOCK
    embeds = [
        e.astype(f32).transpose(1, 0, 2).reshape(CMP_BLOCK, kv_width)
        for e in (key_embed, value_embed)
    ]
    q_blocks = rows // Q_BLOCK
    span_blocks = rows // SEL_BLOCK
    picks = lax.dynamic_slice_in_dim(chosen.astype(jnp.int32), me * q_blocks, q_blocks, 1)
    own_first = (me * q_blocks + jnp.arange(q_blocks, dtype=jnp.int32)) * (Q_BLOCK // SEL_BLOCK)
    usable = picks < own_first[None, :, None]
    span = picks // span_blocks
    slot = (my_z - span // across) * across + (my_x - span % across) % across
    index = jnp.where(usable, slot * span_blocks + picks % span_blocks, 0).reshape(-1)
    bias = jnp.where(usable, 0.0, MASKED).astype(f32)
    bias = jnp.repeat(bias, SEL_BLOCK, axis=-1)
    bias = jnp.pad(bias, ((0, 0), (0, 0), (Q_BLOCK, 0)))[:, :, None, :]

    ranks = lax.axis_size("tp")
    rank_rows = rows // ranks
    key_diag, value_diag = inner_diagonal(key_inner), inner_diagonal(value_inner)
    operands = (
        index,
        bias,
        gain,
        embeds[0],
        block_diagonal(key_outer),
        embeds[1],
        block_diagonal(value_outer),
        tokens,
        mid_weight,
        cosine,
        up,
        down,
        key_diag,
        value_diag,
        *[own.reshape(span_blocks, SEL_BLOCK, LANES) for own in kv],
    )
    vmem = pl.BlockSpec(memory_space=pltpu.VMEM)
    hbm = pl.BlockSpec(memory_space=pl.ANY)
    dma = pltpu.SemaphoreType.DMA
    spread = pltpu.VMEM((kv_local, 2, rows, LANES), bf16)
    gathered = pl.pallas_call(
        functools.partial(exchange_kernel, planes),
        in_specs=[pl.BlockSpec(memory_space=pltpu.SMEM)] + [vmem] * 6 + [hbm] * (7 + kv_local),
        out_specs=vmem,
        out_shape=jax.ShapeDtypeStruct((rank_rows, ranks * kv_local * LANES), bf16),
        scratch_shapes=[pltpu.VMEM((owners * span_blocks, SEL_BLOCK, LANES), bf16)] * kv_local
        + [
            pltpu.VMEM(tokens.shape, bf16),
            pltpu.VMEM(mid_weight.shape, bf16),
            pltpu.VMEM(cosine.shape, f32),
            pltpu.VMEM(cosine.shape, f32),
            pltpu.VMEM(cosine.shape, f32),
            pltpu.VMEM(key_diag.shape, bf16),
            pltpu.VMEM(value_diag.shape, bf16),
            spread,
            spread,
            pltpu.VMEM((rows, kv_width), f32),
            pltpu.VMEM((rows, kv_width), f32),
            pltpu.VMEM((rows, LANES), f32),
            pltpu.VMEM((owners, kv_local, blocks, LANES), bf16),
            pltpu.VMEM((kv_local, rows, LANES), f32),
            pltpu.VMEM((kv_local, rows, LANES), bf16),
            pltpu.VMEM((ranks, kv_local, rank_rows, LANES), bf16),
            dma((7 + kv_local,)),
            dma((kv_local, owners)),
            dma((kv_local, owners)),
            dma((owners,)),
            dma((owners,)),
            dma((kv_local, ranks)),
            dma((kv_local, ranks)),
        ],
        compiler_params=pltpu.CompilerParams(
            collective_id=0, has_side_effects=True, vmem_limit_bytes=60 * 1024 * 1024
        ),
        cost_estimate=cost(4e10, 2e7),
        name="exchange",
    )(*operands)
    return jnp.dot(gathered, out_weight, preferred_element_type=f32).astype(bf16)


def solution(mesh):
    placed = (
        P("kv", None),
        P(),
        P(None, "tp"),
        P(None, "tp"),
        P(None, "tp"),
        P(None, "tp"),
        P(None, "tp"),
        P(),
        P("tp", None, None),
        P("tp", None, None),
        P("tp", None, None),
        P("tp", None, None),
        P("tp", None, None),
        P("tp", None, None),
        P(),
        P("tp", None, None),
    )
    return jax.shard_map(
        per_device, mesh=mesh, in_specs=placed, out_specs=P(("kv", "tp"), None), check_vma=False
    )
```

```python
import functools

import jax
import jax.numpy as jnp
from jax import lax
from jax.experimental import pallas as pl
from jax.experimental.pallas import tpu as pltpu
from jax.sharding import PartitionSpec as P

HEAD_DIM = 64
CMP_BLOCK = 32
SEL_BLOCK = 64
Q_BLOCK = 128
FAR_PICKS = 8
LANES = 2 * HEAD_DIM
PLANES = 4
MESH = pl.DeviceIdType.MESH

ROPE_BASE = 10000.0
norm_eps = 1e-06
MASKED = -1e30

def params(n_axes, limit=48):
    return pltpu.CompilerParams(
        dimension_semantics=("arbitrary",) * n_axes, vmem_limit_bytes=limit * 1024 * 1024
    )


def norm_rows(tok_ref, gain_ref):
    x = tok_ref[...].astype(jnp.float32)
    inv = lax.rsqrt(jnp.mean(x * x, axis=-1, keepdims=True) + norm_eps)
    return (x * inv * gain_ref[...].astype(jnp.float32)).astype(jnp.bfloat16)


def turn(x, cosine, sine_up, sine_down):
    quarter = HEAD_DIM // 2
    return (
        x * cosine
        + pltpu.roll(x, LANES - quarter, 1) * sine_up
        + pltpu.roll(x, quarter, 1) * sine_down
    )


def low_lanes(shape):
    return lax.broadcasted_iota(jnp.int32, shape, 1) < HEAD_DIM


def sel_kernel(tok_ref, gain_ref, w_ref, cos_ref, up_ref, down_ref, *outs):
    normed = norm_rows(tok_ref, gain_ref)
    y = jnp.dot(normed, w_ref[...], preferred_element_type=jnp.float32)
    for k, out in enumerate(outs):
        x = y[:, k * LANES : (k + 1) * LANES]
        low = low_lanes(x.shape)
        turned = turn(x, cos_ref[...], up_ref[...], down_ref[...])
        out[...] = jnp.where(low, turned, x).astype(jnp.bfloat16)


def nt_dot(a, b):
    return lax.dot_general(a, b, (((1,), (1,)), ((), ())), preferred_element_type=jnp.float32)


def gate_lanes(gate, first, shape):
    return jnp.where(low_lanes(shape), gate[:, first : first + 1], gate[:, first + 1 : first + 2])


def merge(out, rows):
    low = low_lanes((rows, LANES))
    return jnp.where(low, pltpu.roll(out[:rows], HEAD_DIM, 1), out[rows:])


def exchange_kernel(
    planes,
    idx_ref,
    bias_ref,
    gain_ref,
    ke_ref,
    ko_ref,
    ve_ref,
    vo_ref,
    tok_hbm,
    w_hbm,
    cos_hbm,
    up_hbm,
    down_hbm,
    ki_hbm,
    vi_hbm,
    *rest,
):
    kv_local = bias_ref.shape[0]
    own_hbm, rest = rest[:kv_local], rest[kv_local:]
    out_ref, rest = rest[0], rest[1:]
    held, rest = rest[:kv_local], rest[kv_local:]
    (
        tok,
        w,
        cosine,
        up,
        down,
        ki,
        vi,
        qp,
        qt,
        ck,
        cv,
        gate,
        sums,
        oc,
        mix,
        got,
        local_sem,
        send_sem,
        recv_sem,
        sum_send,
        sum_recv,
        mix_send,
        mix_recv,
    ) = rest
    owners, ranks = sums.shape[0], got.shape[0]
    rows, width = tok.shape
    span = rows // SEL_BLOCK
    across = owners // planes
    me, rank = lax.axis_index("kv"), lax.axis_index("tp")
    z, x = me // across, me % across

    barrier = pltpu.get_barrier_semaphore()
    for d in range(1, owners):
        pl.semaphore_signal(barrier, inc=1, device_id={"kv": (me + d) % owners}, device_id_type=MESH)
    for d in range(1, ranks):
        pl.semaphore_signal(barrier, inc=1, device_id={"tp": (rank + d) % ranks}, device_id_type=MESH)
    loads = [
        (tok_hbm, tok),
        (w_hbm, w),
        (cos_hbm, cosine),
        (up_hbm, up),
        (down_hbm, down),
        (ki_hbm, ki),
        (vi_hbm, vi),
    ]
    copies = [pltpu.make_async_copy(a, b, local_sem.at[n]) for n, (a, b) in enumerate(loads)]
    for k in range(kv_local):
        copies.append(
            pltpu.make_async_copy(own_hbm[k], held[k].at[pl.ds(0, span)], local_sem.at[len(loads) + k])
        )
    for copy in copies:
        copy.start()
    pl.semaphore_wait(barrier, owners + ranks - 2)

    def slot(k, n):
        return held[k].at[pl.ds(n * span, span)]

    def hop(k, dz, dx):
        n = dz * across + dx
        if dx:
            source = own_hbm[k] if dz == 0 else slot(k, dz * across)
            target = z * across + (x + dx) % across
            sends = (x + dx < across) if dz == 0 else (z >= dz)
            gets = (x >= dx) if dz == 0 else (z >= dz)
        else:
            source = slot(k, (dz - 1) * across) if dz > 1 else own_hbm[k]
            target = lax.rem(me + across, owners)
            sends = (z >= dz - 1) & (z + 1 < planes)
            gets = z >= dz
        copy = pltpu.make_async_remote_copy(
            src_ref=source,
            dst_ref=slot(k, n),
            send_sem=send_sem.at[k, n],
            recv_sem=recv_sem.at[k, n],
            device_id={"kv": target},
            device_id_type=MESH,
        )
        return copy, sends, gets

    def send(k, dz, dx):
        copy, sends, _ = hop(k, dz, dx)
        pl.when(sends)(copy.start)

    def arrive(k, dz, dx):
        copy, _, gets = hop(k, dz, dx)
        pl.when(gets)(copy.wait_recv)

    def send_own(k):
        if planes > 1:
            send(k, 1, 0)
        for dx in range(1, across):
            send(k, 0, dx)

    def forward(k, dz):
        if dz >= planes:
            return
        arrive(k, dz, 0)
        if dz + 1 < planes:
            send(k, dz + 1, 0)
        for dx in range(1, across):
            send(k, dz, dx)

    for k in range(kv_local):
        send_own(k)
    for copy in copies:
        copy.wait()

    tile = 256
    scale = HEAD_DIM ** (-0.5)
    base = kv_local * LANES
    kv_width = kv_local * HEAD_DIM

    def project(i, carry):
        at = pl.ds(pl.multiple_of(i * tile, tile), tile)
        normed = norm_rows(tok.at[at], gain_ref)
        y = jnp.dot(normed, w[...], preferred_element_type=jnp.float32)
        for k in range(kv_local):
            v = y[:, k * LANES : (k + 1) * LANES]
            low = low_lanes(v.shape)
            turned = turn(v, cosine[at], up[at], down[at]) * scale
            for ref, q in ((qp, v * scale), (qt, turned)):
                ref[k, 0, at] = jnp.where(low, q, 0.0).astype(jnp.bfloat16)
                ref[k, 1, at] = jnp.where(low, pltpu.roll(q, HEAD_DIM, 1), 0.0).astype(jnp.bfloat16)
        ck[at] = y[:, base : base + kv_width].astype(jnp.bfloat16).astype(jnp.float32)
        cv[at] = y[:, base + kv_width : base + 2 * kv_width].astype(jnp.bfloat16).astype(jnp.float32)
        gate[at] = jax.nn.sigmoid(y[:, base + 2 * kv_width :])
        return carry

    lax.fori_loop(0, rows // tile, project, 0)

    blocks = rows // CMP_BLOCK

    def summarize(x_ref, e_ref, i_ref, o_ref):
        embed = jnp.concatenate([e_ref[k].astype(jnp.float32) for k in range(kv_local)], axis=1)
        parts = []
        for c in range(CMP_BLOCK):
            part = x_ref[pl.ds(c, blocks, stride=CMP_BLOCK), :] + embed[c : c + 1]
            parts.append(part.astype(jnp.bfloat16))
        flat = jnp.concatenate(parts, axis=1)
        hidden = jnp.dot(flat, inner_diagonal(i_ref[...]), preferred_element_type=jnp.float32)
        hidden = jax.nn.gelu(hidden).astype(jnp.bfloat16)
        return jnp.dot(hidden, block_diagonal(o_ref[...]), preferred_element_type=jnp.float32)

    sk = summarize(ck, ke_ref, ki, ko_ref)
    sv = summarize(cv, ve_ref, vi, vo_ref)
    for k in range(kv_local):
        cut = slice(k * HEAD_DIM, (k + 1) * HEAD_DIM)
        sums[me, k] = jnp.concatenate([sk[:, cut], sv[:, cut]], axis=1).astype(jnp.bfloat16)

    def sum_copy(d, source):
        return pltpu.make_async_remote_copy(
            src_ref=sums.at[source],
            dst_ref=sums.at[source],
            send_sem=sum_send.at[d],
            recv_sem=sum_recv.at[d],
            device_id={"kv": (me + d) % owners},
            device_id_type=MESH,
        )

    for d in range(1, owners):
        sum_copy(d, me).start()
    for k in range(kv_local):
        forward(k, 1)
    for d in range(1, owners):
        sum_copy(d, (me + owners - d) % owners).wait_recv()

    def compress(i, carry):
        at = pl.ds(pl.multiple_of(i * tile, tile), tile)
        row = lax.broadcasted_iota(jnp.int32, (2 * tile, 1), 0)
        pos = me * rows + i * tile + jnp.where(row >= tile, row - tile, row)
        lane = lax.broadcasted_iota(jnp.int32, (1, owners * blocks), 1)
        allowed = (lane + 1) * CMP_BLOCK - 1 <= pos
        for k in range(kv_local):
            keys = jnp.concatenate([sums[s, k] for s in range(owners)], axis=0)
            q = jnp.concatenate([qp[k, 0, at], qp[k, 1, at]], axis=0)
            s = jnp.where(allowed, nt_dot(q, keys), MASKED)
            top = jnp.max(s, axis=-1, keepdims=True)
            e = jnp.where(allowed, jnp.exp(s - top), 0.0)
            total = jnp.sum(e, axis=-1, keepdims=True)
            o = jnp.dot(e.astype(jnp.bfloat16), keys, preferred_element_type=jnp.float32)
            o = o * jnp.where(total > 0.0, 1.0 / jnp.where(total > 0.0, total, 1.0), 0.0)
            o = merge(o, tile)
            oc[k, at] = o * gate_lanes(gate[at], 2 * k, o.shape)
        return carry

    tiles = rows // tile
    bounds = [tiles * k // kv_local for k in range(kv_local + 1)]
    for k in range(kv_local):
        lax.fori_loop(bounds[k], bounds[k + 1], compress, 0)
        forward(k, 2)
    for dz in range(3, planes):
        for k in range(kv_local):
            forward(k, dz)

    rank_rows = rows // ranks
    group = rank_rows // Q_BLOCK
    q_blocks = rows // Q_BLOCK
    half_gates = 2 * kv_local

    def mix_copy(k, step):
        target = (rank + 1 + step) % ranks
        at = pl.ds(pl.multiple_of(target * rank_rows, rank_rows), rank_rows)
        return pltpu.make_async_remote_copy(
            src_ref=mix.at[k, at],
            dst_ref=got.at[rank, k],
            send_sem=mix_send.at[k, step],
            recv_sem=mix_recv.at[k, step],
            device_id={"tp": target},
            device_id_type=MESH,
        )

    def choose(k):
        def one(step, carry):
            target = (rank + 1 + step) % ranks
            for u in range(group):
                j = target * group + u
                at = pl.ds(pl.multiple_of(j * Q_BLOCK, Q_BLOCK), Q_BLOCK)
                own = j * (Q_BLOCK // SEL_BLOCK)
                parts = [held[k][own + b] for b in range(Q_BLOCK // SEL_BLOCK)]
                for a in range(FAR_PICKS):
                    pick = idx_ref[(k * q_blocks + j) * FAR_PICKS + a]
                    parts.append(held[k][pick])
                keys = jnp.concatenate(parts, axis=0)
                q = jnp.concatenate([qt[k, 0, at], qt[k, 1, at]], axis=0)
                s = nt_dot(q, keys) + bias_ref[k, j]
                row = lax.broadcasted_iota(jnp.int32, (2 * Q_BLOCK, Q_BLOCK), 0)
                row = jnp.where(row >= Q_BLOCK, row - Q_BLOCK, row)
                lane = lax.broadcasted_iota(jnp.int32, row.shape, 1)
                near = jnp.where(lane > row, MASKED, s[:, :Q_BLOCK])
                s = jnp.concatenate([near, s[:, Q_BLOCK:]], axis=1)
                top = jnp.max(s, axis=-1, keepdims=True)
                e = jnp.exp(s - top)
                total = jnp.sum(e, axis=-1, keepdims=True)
                o = jnp.dot(e.astype(jnp.bfloat16), keys, preferred_element_type=jnp.float32)
                o = merge(o * (1.0 / total), Q_BLOCK)
                g = gate_lanes(gate[at], half_gates + 2 * k, o.shape)
                mix[k, at] = (oc[k, at] + o * g).astype(jnp.bfloat16)
            pl.when(step > 0)(lambda: mix_copy(k, step - 1).start())
            return carry

        lax.fori_loop(0, ranks, one, 0)

    moves = [(dz, dx) for dz in range(planes) for dx in range(across) if (dz, dx) != (0, 0)]
    for k in range(kv_local):
        for dz, dx in moves:
            if dx:
                arrive(k, dz, dx)
        choose(k)
    own_at = pl.ds(pl.multiple_of(rank * rank_rows, rank_rows), rank_rows)
    for k in range(kv_local):
        for dz, dx in moves:
            copy, sends, _ = hop(k, dz, dx)
            pl.when(sends)(copy.wait_send)
    for d in range(1, owners):
        sum_copy(d, me).wait_send()
    for k in range(kv_local):
        got[rank, k] = mix[k, own_at]
        for step in range(ranks - 1):
            mix_copy(k, step).wait_send()
            mix_copy(k, step).wait_recv()
    for t in range(ranks):
        for k in range(kv_local):
            first = (t * kv_local + k) * LANES
            out_ref[:, first : first + LANES] = got[t, k]


def cost(flops, moved):
    return pl.CostEstimate(flops=int(flops), bytes_accessed=int(moved), transcendentals=0)


def block_diagonal(w):
    n, a, b = w.shape
    zero = jnp.zeros((a, b), w.dtype)
    return jnp.concatenate(
        [jnp.concatenate([w[i] if i == j else zero for j in range(n)], axis=1) for i in range(n)],
        axis=0,
    )


def inner_diagonal(w):
    n, _, e = w.shape
    zero = jnp.zeros((HEAD_DIM, e), w.dtype)
    parts = []
    for c in range(CMP_BLOCK):
        for i in range(n):
            cut = w[i, c * HEAD_DIM : (c + 1) * HEAD_DIM]
            parts.append(jnp.concatenate([cut if i == j else zero for j in range(n)], axis=1))
    return jnp.concatenate(parts, axis=0)


def per_device(
    tokens,
    norm_gain,
    query_weight,
    cmp_key_weight,
    cmp_value_weight,
    sel_key_weight,
    sel_value_weight,
    branch_weight,
    key_embed,
    key_inner,
    key_outer,
    value_embed,
    value_inner,
    value_outer,
    out_weight,
    chosen,
):
    rows, width = tokens.shape
    kv_local = key_embed.shape[0]
    heads_local = query_weight.shape[1] // HEAD_DIM
    owners = lax.axis_size("kv")
    me = lax.axis_index("kv")
    planes = PLANES if owners % PLANES == 0 else 1
    across = owners // planes
    my_z, my_x = me // across, me % across
    offset = me * rows
    f32 = jnp.float32
    bf16 = jnp.bfloat16

    half = HEAD_DIM // 2
    lane = jnp.arange(LANES, dtype=jnp.int32)
    inverse = ROPE_BASE ** (-(lane % half).astype(f32) / half)
    positions = offset + jnp.arange(rows, dtype=jnp.int32)
    phases = positions.astype(f32)[:, None] * inverse[None, :]
    cosine = jnp.cos(phases)
    sine = jnp.sin(phases)
    first = (lane % HEAD_DIM < half)[None, :]
    up = jnp.where(first, -sine, 0.0)
    down = jnp.where(first, 0.0, sine)
    gain = norm_gain.reshape(1, width)

    def heads_of(w, k):
        return w[:, k * HEAD_DIM : (k + 1) * HEAD_DIM]

    sel_weight = jnp.concatenate(
        [heads_of(w, k) for k in range(kv_local) for w in (sel_key_weight, sel_value_weight)],
        axis=1,
    )
    tile = 256
    steps = rows // tile
    row_spec = lambda cols: pl.BlockSpec((tile, cols), lambda i: (i, 0))
    full = lambda shape: pl.BlockSpec(shape, lambda *_: (0,) * len(shape))
    kv = pl.pallas_call(
        sel_kernel,
        grid=(steps,),
        in_specs=[row_spec(width), full((1, width)), full(sel_weight.shape)]
        + [row_spec(LANES)] * 3,
        out_specs=[row_spec(LANES)] * kv_local,
        out_shape=[jax.ShapeDtypeStruct((rows, LANES), bf16)] * kv_local,
        compiler_params=params(1),
        cost_estimate=cost(2 * rows * width * sel_weight.shape[1], rows * width * 2),
        name="sel_project",
    )(tokens, gain, sel_weight, cosine, up, down)

    gate_cols = lax.dynamic_slice_in_dim(
        branch_weight, lax.axis_index("tp") * heads_local, heads_local, 2
    )
    gate_weight = jnp.concatenate([gate_cols[0], gate_cols[1]], axis=1)
    gate_count = 2 * heads_local
    mid_weight = jnp.concatenate(
        [query_weight, cmp_key_weight, cmp_value_weight, jnp.pad(gate_weight, ((0, 0), (0, LANES - gate_count)))],
        axis=1,
    )
    kv_width = kv_local * HEAD_DIM
    blocks = rows // CMP_BLOCK
    q_blocks = rows // Q_BLOCK
    span_blocks = rows // SEL_BLOCK
    picks = lax.dynamic_slice_in_dim(chosen.astype(jnp.int32), me * q_blocks, q_blocks, 1)
    own_first = (me * q_blocks + jnp.arange(q_blocks, dtype=jnp.int32)) * (Q_BLOCK // SEL_BLOCK)
    usable = picks < own_first[None, :, None]
    span = picks // span_blocks
    slot = (my_z - span // across) * across + (my_x - span % across) % across
    index = jnp.where(usable, slot * span_blocks + picks % span_blocks, 0).reshape(-1)
    bias = jnp.where(usable, 0.0, MASKED).astype(f32)
    bias = jnp.repeat(bias, SEL_BLOCK, axis=-1)
    bias = jnp.pad(bias, ((0, 0), (0, 0), (Q_BLOCK, 0)))[:, :, None, :]

    ranks = lax.axis_size("tp")
    rank_rows = rows // ranks
    operands = (
        index,
        bias,
        gain,
        key_embed,
        key_outer,
        value_embed,
        value_outer,
        tokens,
        mid_weight,
        cosine,
        up,
        down,
        key_inner,
        value_inner,
        *[own.reshape(span_blocks, SEL_BLOCK, LANES) for own in kv],
    )
    vmem = pl.BlockSpec(memory_space=pltpu.VMEM)
    hbm = pl.BlockSpec(memory_space=pl.ANY)
    dma = pltpu.SemaphoreType.DMA
    spread = pltpu.VMEM((kv_local, 2, rows, LANES), bf16)
    gathered = pl.pallas_call(
        functools.partial(exchange_kernel, planes),
        in_specs=[pl.BlockSpec(memory_space=pltpu.SMEM)] + [vmem] * 6 + [hbm] * (7 + kv_local),
        out_specs=vmem,
        out_shape=jax.ShapeDtypeStruct((rank_rows, ranks * kv_local * LANES), bf16),
        scratch_shapes=[pltpu.VMEM((owners * span_blocks, SEL_BLOCK, LANES), bf16)] * kv_local
        + [
            pltpu.VMEM(tokens.shape, bf16),
            pltpu.VMEM(mid_weight.shape, bf16),
            pltpu.VMEM(cosine.shape, f32),
            pltpu.VMEM(cosine.shape, f32),
            pltpu.VMEM(cosine.shape, f32),
            pltpu.VMEM(key_inner.shape, bf16),
            pltpu.VMEM(value_inner.shape, bf16),
            spread,
            spread,
            pltpu.VMEM((rows, kv_width), f32),
            pltpu.VMEM((rows, kv_width), f32),
            pltpu.VMEM((rows, LANES), f32),
            pltpu.VMEM((owners, kv_local, blocks, LANES), bf16),
            pltpu.VMEM((kv_local, rows, LANES), f32),
            pltpu.VMEM((kv_local, rows, LANES), bf16),
            pltpu.VMEM((ranks, kv_local, rank_rows, LANES), bf16),
            dma((7 + kv_local,)),
            dma((kv_local, owners)),
            dma((kv_local, owners)),
            dma((owners,)),
            dma((owners,)),
            dma((kv_local, ranks)),
            dma((kv_local, ranks)),
        ],
        compiler_params=pltpu.CompilerParams(
            collective_id=0, has_side_effects=True, vmem_limit_bytes=60 * 1024 * 1024
        ),
        cost_estimate=cost(4e10, 2e7),
        name="exchange",
    )(*operands)
    return jnp.dot(gathered, out_weight, preferred_element_type=f32).astype(bf16)


def solution(mesh):
    placed = (
        P("kv", None),
        P(),
        P(None, "tp"),
        P(None, "tp"),
        P(None, "tp"),
        P(None, "tp"),
        P(None, "tp"),
        P(),
        P("tp", None, None),
        P("tp", None, None),
        P("tp", None, None),
        P("tp", None, None),
        P("tp", None, None),
        P("tp", None, None),
        P(),
        P("tp", None, None),
    )
    return jax.shard_map(
        per_device, mesh=mesh, in_specs=placed, out_specs=P(("kv", "tp"), None), check_vma=False
    )
```
